32 devices in a mesh: rep: 2 (over x), fs: 8 (over z, y), tp: 2 (over core).
Axes of the slice: x: 2, y: 2, z: 4, core: 2. Of those that a mesh axis runs over, the one named last changes fastest.
Arguments:
- input_activation_entries: bfloat16 [6144, 2048], P(('rep', 'fs')), may hold values from -6 to 6
- premixing_rescale_factor: float32 [2048], replicated, may hold values from 0.1 to 1.9
- probe_weight_table: float32 [2048, 1024], P('fs', 'tp'), may hold values from -0.125 to 0.125
- probe_factor_list: float32 [1024], P('tp'), may hold values from 0.5 to 2
- lookup_weight_table: float32 [2048, 1024], P('fs', 'tp'), may hold values from -0.125 to 0.125
- lookup_factor_list: float32 [1024], P('tp'), may hold values from 0.5 to 2
- forget_weight_table: float32 [2048, 1024], P('fs', 'tp'), may hold values from -0.125 to 0.125
- forget_factor_list: float32 [1024], P('tp'), may hold values from 1 to 8
- forget_shift_term: float32 [1024], P('tp'), may hold values from -3 to 7
- extra_forget_logs: float32 [6144, 8], P(('rep', 'fs'), 'tp'), may hold values from -0.7 to 0
- content_weight_table: float32 [2048, 2048], P('fs', 'tp'), may hold values from -0.125 to 0.125
- content_factor_list: float32 [2048], P('tp'), may hold values from 0.5 to 2
- filter_weight_table: float32 [2048, 2048], P('fs', 'tp'), may hold values from -0.125 to 0.125
- filter_factor_list: float32 [2048], P('tp'), may hold values from 0.5 to 2
- per_group_rescale_factor: float32 [2048], P('tp'), may hold values from 0.1 to 1.9
- emission_weight_table: float32 [2048, 2048], P('tp', 'fs'), may hold values from -0.125 to 0.125
- emission_factor_list: float32 [2048], P('fs'), may hold values from 0.5 to 2
- perceptron_prenorm_factor: float32 [2048], replicated, may hold values from 0.1 to 1.9
- raising_weight_table: float32 [2048, 8192], P('fs', 'tp'), may hold values from -0.125 to 0.125
- raising_factor_list: float32 [8192], P('tp'), may hold values from 0.5 to 2
- lowering_weight_table: float32 [8192, 2048], P('tp', 'fs'), may hold values from -0.0625 to 0.0625
- lowering_factor_list: float32 [2048], P('fs'), may hold values from 0.5 to 2
Outputs:
- layer_out: bfloat16 [6144, 2048], P(('rep', 'fs'))
The draws below stay inside these ranges and needn't reach their ends.
All inputs are finite; a program needn't handle non-finite values.
Results may differ from the reference program's by a relative error of at most 0.02.
Values may be sent and summed in bfloat16 or wider, within the bound.
A program may use at most 128 MiB of HBM per device.

```python
import math
import jax
import jax.numpy as jnp
from jax import lax

D = 2048
HEADS = 8
LOOKUP_FEATURES = 128
FF = 8192
BLOCK = 64
TOK_DEV = 384
KW = 1024
VW = 2048
TOKENS = 6144
N_TP = 2


def draw_forget_shift_term(key, part):
    head_key, slow_key, fast_key = jax.random.split(key, 3)
    odds = 2
    fast_head = jax.random.randint(head_key, (HEADS,), 0, odds) == 0
    fast_channel = jnp.repeat(fast_head, LOOKUP_FEATURES)
    slow_value = jax.random.uniform(slow_key, (KW,), jnp.float32, 5.0, 7.0)
    fast_value = jax.random.uniform(fast_key, (KW,), jnp.float32, -3.0, -1.0)
    return jnp.where(fast_channel, fast_value, slow_value)


def draw_extra_forget_logs(key, part):
    rate_key, place_key, depth_key = jax.random.split(key, 3)
    blocks = TOKENS // BLOCK
    lowest = 0.0001
    rates = jnp.exp(jax.random.uniform(rate_key, (blocks, HEADS), jnp.float32, jnp.log(lowest), jnp.log(0.003)))
    base = -jnp.repeat(rates, BLOCK, axis=0)
    hits = jax.random.randint(place_key, (TOKENS, HEADS), 0, TOK_DEV) < 3
    depth = jnp.log(jax.random.uniform(depth_key, (TOKENS, HEADS), jnp.float32, 0.5, 0.8))
    return base + jnp.where(hits, depth, 0.0)


def levels(key, extent, cuts, least, largest):
    def one(position, shards_of):
        steps = jax.random.uniform(jax.random.fold_in(jax.random.fold_in(key, 6), position), (shards_of,), jnp.float32, least / len(cuts), largest / len(cuts))
        return jnp.repeat(jnp.exp(steps), extent[position] // shards_of).reshape((-1,) + (1,) * (len(extent) - position - 1))

    level = one(*cuts[0])
    for cut in cuts[1:]:
        level = level * one(*cut)
    return level


def noise(own_key, extent, scale, reach, shards=(), held_as=jnp.bfloat16):
    factor_of = levels(own_key, extent, shards, -0.22, 0.18) if shards else 1.0
    array = jax.random.normal(own_key, extent, jnp.float32) * scale * factor_of
    return jnp.minimum(jnp.maximum(array, -reach), reach).astype(held_as)


def setup_inputs(seed: int = 0) -> dict:
    key_of = jax.random.split(jax.random.key(seed), 23)
    input_activation_entries = noise(key_of[0], (TOKENS, D), 1.0, 6.0, ((0, 16),))
    premixing_rescale_factor = jnp.clip(1.0 + 0.18 * jax.random.normal(key_of[1], (D,), jnp.float32), 0.1, 1.9)
    probe_weight_table = noise(key_of[2], (D, KW), D ** -0.5, 0.125, ((0, 8), (1, 2)), jnp.float32)
    probe_factor_list = jnp.clip(jnp.exp(math.log(2.0) - 1.3862944 * jax.random.uniform(key_of[3], (KW,), jnp.float32) ** levels(key_of[3], (KW,), ((0, 2),), -0.2, 0.2)), 0.5, 2.0)
    lookup_weight_table = noise(key_of[4], (D, KW), D ** -0.5, 0.125, ((0, 8), (1, 2)), jnp.float32)
    lookup_factor_list = jnp.clip(jnp.exp(math.log(2.0) - 1.3862944 * jax.random.uniform(key_of[5], (KW,), jnp.float32) ** levels(key_of[5], (KW,), ((0, 2),), -0.2, 0.2)), 0.5, 2.0)
    forget_weight_table = noise(key_of[6], (D, KW), D ** -0.5, 0.125, ((0, 8), (1, 2)), jnp.float32)
    forget_factor_list = jnp.clip(jnp.exp(math.log(8.0) - 2.0794415 * jax.random.uniform(key_of[7], (KW,), jnp.float32) ** levels(key_of[7], (KW,), ((0, 2),), -0.2, 0.2)), 1.0, 8.0)
    forget_shift_term = draw_forget_shift_term(jax.random.fold_in(key_of[22], 71), 0)
    extra_forget_logs = draw_extra_forget_logs(jax.random.fold_in(key_of[22], 71), 0)
    content_weight_table = noise(key_of[10], (D, VW), D ** -0.5, 0.125, ((0, 8), (1, 2)), jnp.float32)
    content_factor_list = jnp.clip(jnp.exp(math.log(2.0) - 1.3862944 * jax.random.uniform(key_of[11], (VW,), jnp.float32) ** levels(key_of[11], (VW,), ((0, 2),), -0.2, 0.2)), 0.5, 2.0)
    filter_weight_table = noise(key_of[12], (D, VW), D ** -0.5, 0.125, ((0, 8), (1, 2)), jnp.float32)
    filter_factor_list = jnp.clip(jnp.exp(math.log(2.0) - 1.3862944 * jax.random.uniform(key_of[13], (VW,), jnp.float32) ** levels(key_of[13], (VW,), ((0, 2),), -0.2, 0.2)), 0.5, 2.0)
    per_group_rescale_factor = jnp.clip(1.0 + 0.18 * jax.random.normal(key_of[14], (VW,), jnp.float32), 0.1, 1.9)
    emission_weight_table = noise(key_of[15], (VW, D), VW ** -0.5, 0.125, ((0, 2), (1, 8)), jnp.float32)
    emission_factor_list = jnp.clip(jnp.exp(math.log(2.0) - 1.3862944 * jax.random.uniform(key_of[16], (D,), jnp.float32) ** levels(key_of[16], (D,), ((0, 8),), -0.2, 0.2)), 0.5, 2.0)
    perceptron_prenorm_factor = jnp.clip(1.0 + 0.18 * jax.random.normal(key_of[17], (D,), jnp.float32), 0.1, 1.9)
    raising_weight_table = noise(key_of[18], (D, FF), D ** -0.5, 0.125, ((0, 8), (1, 2)), jnp.float32)
    raising_factor_list = jnp.clip(jnp.exp(math.log(2.0) - 1.3862944 * jax.random.uniform(key_of[19], (FF,), jnp.float32) ** levels(key_of[19], (FF,), ((0, 2),), -0.2, 0.2)), 0.5, 2.0)
    lowering_weight_table = noise(key_of[20], (FF, D), FF ** -0.5, 0.0625, ((0, 2), (1, 8)), jnp.float32)
    lowering_factor_list = jnp.clip(jnp.exp(math.log(2.0) - 1.3862944 * jax.random.uniform(key_of[21], (D,), jnp.float32) ** levels(key_of[21], (D,), ((0, 8),), -0.2, 0.2)), 0.5, 2.0)
    return {"input_activation_entries": input_activation_entries, "premixing_rescale_factor": premixing_rescale_factor, "probe_weight_table": probe_weight_table, "probe_factor_list": probe_factor_list, "lookup_weight_table": lookup_weight_table, "lookup_factor_list": lookup_factor_list, "forget_weight_table": forget_weight_table, "forget_factor_list": forget_factor_list, "forget_shift_term": forget_shift_term, "extra_forget_logs": extra_forget_logs, "content_weight_table": content_weight_table, "content_factor_list": content_factor_list, "filter_weight_table": filter_weight_table, "filter_factor_list": filter_factor_list, "per_group_rescale_factor": per_group_rescale_factor, "emission_weight_table": emission_weight_table, "emission_factor_list": emission_factor_list, "perceptron_prenorm_factor": perceptron_prenorm_factor, "raising_weight_table": raising_weight_table, "raising_factor_list": raising_factor_list, "lowering_weight_table": lowering_weight_table, "lowering_factor_list": lowering_factor_list}


epsilon = 1e-06
filter_rescaled_entries = 16.0
highest = lax.Precision.HIGHEST

def rms_rows(matrix, gain):
    matrix = matrix.astype(jnp.float32)
    return matrix * lax.rsqrt(lax.optimization_barrier(jnp.mean(matrix * matrix, axis=-1, keepdims=True)) + epsilon) * gain

def recur_head(queries, keys_in, vals, forget_log_rate):
    length = queries.shape[0]
    blocks = length // BLOCK

    def to_blocks(tensor):
        return tensor.astype(jnp.float32).reshape(blocks, BLOCK, tensor.shape[-1])
    causal = jnp.tril(jnp.ones((BLOCK, BLOCK), dtype=bool))[:, :, None]

    def advance(memory, inputs):
        query_block, key_block, value_block, decay_block = inputs
        cumulative = jnp.cumsum(decay_block, axis=0)
        spread = cumulative[:, None, :] - cumulative[None, :, :]
        weights = jnp.exp(jnp.where(causal, spread, -jnp.inf))
        scores = jnp.einsum('tc,sc,tsc->ts', query_block, key_block, weights, precision=highest)
        within = jnp.dot(scores, value_block, precision=highest)
        carried = jnp.dot(query_block * jnp.exp(cumulative), memory, precision=highest)
        closing = cumulative[-1]
        scaled_keys = key_block * jnp.exp(closing[None, :] - cumulative)
        memory = jnp.exp(closing)[:, None] * memory + jnp.dot(scaled_keys.T, value_block, precision=highest)
        return (memory, within + carried)
    initial = jnp.zeros((queries.shape[-1], vals.shape[-1]), jnp.float32)
    _, outputs = lax.scan(advance, initial, (to_blocks(queries), to_blocks(keys_in), to_blocks(vals), to_blocks(forget_log_rate)))
    return outputs.reshape(length, vals.shape[-1])

def per_group_mixing_values(probe_mapped_entries, lookup_mapped_entries, forget_mapped_entries, content_mapped_entries, filter_mapped_entries, forget_shift_term, extra_forget_logs, per_group_rescale_factor):
    group_count_total = extra_forget_logs.shape[-1]
    queries = (jax.nn.silu(probe_mapped_entries) * LOOKUP_FEATURES ** (-0.5)).astype(jnp.bfloat16)
    keyed = jax.nn.silu(lookup_mapped_entries).astype(jnp.bfloat16)
    valued = jax.nn.silu(content_mapped_entries).astype(jnp.bfloat16)
    forget_log_rate = jax.nn.log_sigmoid(forget_mapped_entries + forget_shift_term) / filter_rescaled_entries + jnp.repeat(extra_forget_logs, LOOKUP_FEATURES, axis=1)

    def by_head(tensor):
        return tensor.reshape(tensor.shape[0], group_count_total, -1).transpose(1, 0, 2)
    outputs = jax.vmap(recur_head)(by_head(queries), by_head(keyed), by_head(valued), by_head(forget_log_rate))
    outputs = outputs * lax.rsqrt(lax.optimization_barrier(jnp.mean(outputs * outputs, axis=-1, keepdims=True)) + epsilon)
    merged = outputs.transpose(1, 0, 2).reshape(outputs.shape[1], -1)
    return (merged * per_group_rescale_factor * jax.nn.silu(filter_mapped_entries)).astype(jnp.bfloat16)

def grouped_sum(rows, weight, scale):
    rows_per = weight.shape[0] // N_TP
    running = jnp.zeros((rows.shape[0], weight.shape[1]), jnp.float32)
    for member in range(N_TP):
        piece = jnp.dot(rows[:, member * rows_per:(member + 1) * rows_per], weight[member * rows_per:(member + 1) * rows_per].astype(jnp.bfloat16), preferred_element_type=jnp.float32) * scale
        rounded = lax.optimization_barrier(piece.astype(jnp.bfloat16))
        running = running + rounded.astype(jnp.float32)
    return running

def reference(input_activation_entries, premixing_rescale_factor, probe_weight_table, probe_factor_list, lookup_weight_table, lookup_factor_list, forget_weight_table, forget_factor_list, forget_shift_term, extra_forget_logs, content_weight_table, content_factor_list, filter_weight_table, filter_factor_list, per_group_rescale_factor, emission_weight_table, emission_factor_list, perceptron_prenorm_factor, raising_weight_table, raising_factor_list, lowering_weight_table, lowering_factor_list):
    normed = rms_rows(input_activation_entries, premixing_rescale_factor).astype(jnp.bfloat16)

    def project(weight, scale):
        return jnp.dot(normed, weight.astype(jnp.bfloat16), preferred_element_type=jnp.float32) * scale
    probe_mapped_entries = project(probe_weight_table, probe_factor_list)
    lookup_mapped_entries = project(lookup_weight_table, lookup_factor_list)
    forget_mapped_entries = project(forget_weight_table, forget_factor_list)
    content_mapped_entries = project(content_weight_table, content_factor_list)
    filter_mapped_entries = project(filter_weight_table, filter_factor_list)
    seq_count = input_activation_entries.shape[0] // TOK_DEV

    def batched_by_stream(tensor):
        return tensor.reshape(seq_count, TOK_DEV, tensor.shape[-1])

    def per_stream_layout(pieces):
        return per_group_mixing_values(pieces[0], pieces[1], pieces[2], pieces[3], pieces[4], forget_shift_term, pieces[5], per_group_rescale_factor)
    mixing_product = lax.map(per_stream_layout, (batched_by_stream(probe_mapped_entries), batched_by_stream(lookup_mapped_entries), batched_by_stream(forget_mapped_entries), batched_by_stream(content_mapped_entries), batched_by_stream(filter_mapped_entries), batched_by_stream(extra_forget_logs)))
    mixing_product = mixing_product.reshape(input_activation_entries.shape[0], -1)
    mix_sum = grouped_sum(mixing_product, emission_weight_table, emission_factor_list)
    residual = (input_activation_entries.astype(jnp.float32) + mix_sum).astype(jnp.bfloat16)
    normed_mlp = rms_rows(residual, perceptron_prenorm_factor).astype(jnp.bfloat16)
    lifted = jnp.dot(normed_mlp, raising_weight_table.astype(jnp.bfloat16), preferred_element_type=jnp.float32) * raising_factor_list
    hidden = jnp.square(jax.nn.relu(lifted)).astype(jnp.bfloat16)
    mlp_sum = grouped_sum(hidden, lowering_weight_table, lowering_factor_list)
    return (residual.astype(jnp.float32) + mlp_sum).astype(jnp.bfloat16)
```

```python
import jax
import jax.numpy as jnp
from jax import lax
from jax.sharding import Mesh, PartitionSpec as P

LOOKUP_FEATURES = 128
BLOCK = 64
GROUP = 4


epsilon = 1e-06
filter_rescaled_entries = 16.0
highest = lax.Precision.HIGHEST


def rms_rows(matrix, gain):
    matrix = matrix.astype(jnp.float32)
    return matrix * lax.rsqrt(jnp.mean(matrix * matrix, axis=-1, keepdims=True) + epsilon) * gain


def recur_head(queries, keys_in, vals, forget_log_rate):
    length = queries.shape[0]
    blocks = length // BLOCK

    def to_blocks(tensor):
        return tensor.astype(jnp.float32).reshape(blocks, BLOCK, tensor.shape[-1])

    causal = jnp.tril(jnp.ones((BLOCK, BLOCK), dtype=bool))[:, :, None]

    def advance(memory, inputs):
        query_block, key_block, value_block, decay_block = inputs
        cumulative = jnp.cumsum(decay_block, axis=0)
        spread = cumulative[:, None, :] - cumulative[None, :, :]
        weights = jnp.exp(jnp.where(causal, spread, -jnp.inf))
        scores = jnp.einsum("tc,sc,tsc->ts", query_block, key_block, weights, precision=highest)
        within = jnp.dot(scores, value_block, precision=highest)
        carried = jnp.dot(query_block * jnp.exp(cumulative), memory, precision=highest)
        closing = cumulative[-1]
        scaled_keys = key_block * jnp.exp(closing[None, :] - cumulative)
        memory = jnp.exp(closing)[:, None] * memory + jnp.dot(
            scaled_keys.T, value_block, precision=highest
        )
        return (memory, within + carried)

    initial = jnp.zeros((queries.shape[-1], vals.shape[-1]), jnp.float32)
    _, outputs = lax.scan(
        advance,
        initial,
        (to_blocks(queries), to_blocks(keys_in), to_blocks(vals), to_blocks(forget_log_rate)),
    )
    return outputs.reshape(length, vals.shape[-1])


def per_group_mixing_values(
    probe_mapped_entries,
    lookup_mapped_entries,
    forget_mapped_entries,
    content_mapped_entries,
    filter_mapped_entries,
    forget_shift_term,
    extra_forget_logs,
    per_group_rescale_factor,
):
    group_count_total = extra_forget_logs.shape[-1]
    queries = (jax.nn.silu(probe_mapped_entries) * LOOKUP_FEATURES ** (-0.5)).astype(jnp.bfloat16)
    keyed = jax.nn.silu(lookup_mapped_entries).astype(jnp.bfloat16)
    valued = jax.nn.silu(content_mapped_entries).astype(jnp.bfloat16)
    forget_log_rate = jax.nn.log_sigmoid(
        forget_mapped_entries + forget_shift_term
    ) / filter_rescaled_entries + jnp.repeat(extra_forget_logs, LOOKUP_FEATURES, axis=1)

    def by_head(tensor):
        return tensor.reshape(tensor.shape[0], group_count_total, -1).transpose(1, 0, 2)

    outputs = jax.vmap(recur_head)(
        by_head(queries), by_head(keyed), by_head(valued), by_head(forget_log_rate)
    )
    outputs = outputs * lax.rsqrt(jnp.mean(outputs * outputs, axis=-1, keepdims=True) + epsilon)
    merged = outputs.transpose(1, 0, 2).reshape(outputs.shape[1], -1)
    return (merged * per_group_rescale_factor * jax.nn.silu(filter_mapped_entries)).astype(
        jnp.bfloat16
    )


def plain_body(
    input_activation_entries,
    premixing_rescale_factor,
    probe_weight_table,
    probe_factor_list,
    lookup_weight_table,
    lookup_factor_list,
    forget_weight_table,
    forget_factor_list,
    forget_shift_term,
    extra_forget_logs,
    content_weight_table,
    content_factor_list,
    filter_weight_table,
    filter_factor_list,
    per_group_rescale_factor,
    emission_weight_table,
    emission_factor_list,
    perceptron_prenorm_factor,
    raising_weight_table,
    raising_factor_list,
    lowering_weight_table,
    lowering_factor_list,
):
    whole_out_scale, whole_down_scale = (
        lax.all_gather(emission_factor_list, "fs", axis=0, tiled=True),
        lax.all_gather(lowering_factor_list, "fs", axis=0, tiled=True),
    )
    normed = rms_rows(input_activation_entries, premixing_rescale_factor).astype(jnp.bfloat16)
    query_bf = probe_weight_table.astype(jnp.bfloat16)
    key_bf = lookup_weight_table.astype(jnp.bfloat16)
    decay_bf = forget_weight_table.astype(jnp.bfloat16)
    value_bf = content_weight_table.astype(jnp.bfloat16)
    gate_bf = filter_weight_table.astype(jnp.bfloat16)
    out_bf = emission_weight_table.astype(jnp.bfloat16)
    up_bf = raising_weight_table.astype(jnp.bfloat16)
    down_bf = lowering_weight_table.astype(jnp.bfloat16)
    pieces = (
        lax.all_gather(query_bf, "fs", axis=0, tiled=True),
        lax.all_gather(key_bf, "fs", axis=0, tiled=True),
        lax.all_gather(decay_bf, "fs", axis=0, tiled=True),
        lax.all_gather(value_bf, "fs", axis=0, tiled=True),
        lax.all_gather(gate_bf, "fs", axis=0, tiled=True),
    )
    columns = normed
    projected = tuple(
        (
            jnp.dot(columns, shard_piece, preferred_element_type=jnp.float32)
            for shard_piece in pieces
        )
    )
    mixing_product = per_group_mixing_values(
        projected[0] * probe_factor_list,
        projected[1] * lookup_factor_list,
        projected[2] * forget_factor_list,
        projected[3] * content_factor_list,
        projected[4] * filter_factor_list,
        forget_shift_term,
        extra_forget_logs,
        per_group_rescale_factor,
    )
    column_scale = whole_out_scale
    mix_part = (
        jnp.dot(
            mixing_product,
            lax.all_gather(out_bf, "fs", axis=1, tiled=True),
            preferred_element_type=jnp.float32,
        )
        * column_scale
    )
    mix_rounded = lax.optimization_barrier(mix_part.astype(jnp.bfloat16)).astype(jnp.float32)
    mix_sum = lax.psum(mix_rounded.astype(jnp.bfloat16), "tp").astype(jnp.float32)
    residual = (input_activation_entries.astype(jnp.float32) + mix_sum).astype(jnp.bfloat16)
    normed_mlp = rms_rows(residual, perceptron_prenorm_factor).astype(jnp.bfloat16)
    columns = normed_mlp
    lifted = jnp.dot(
        columns, lax.all_gather(up_bf, "fs", axis=0, tiled=True), preferred_element_type=jnp.float32
    )
    hidden = jnp.square(jax.nn.relu(lifted * raising_factor_list)).astype(jnp.bfloat16)
    column_scale = whole_down_scale
    mlp_part = (
        jnp.dot(
            hidden,
            lax.all_gather(down_bf, "fs", axis=1, tiled=True),
            preferred_element_type=jnp.float32,
        )
        * column_scale
    )
    mlp_rounded = lax.optimization_barrier(mlp_part.astype(jnp.bfloat16)).astype(jnp.float32)
    mlp_sum = lax.psum(mlp_rounded.astype(jnp.bfloat16), "tp").astype(jnp.float32)
    return (residual.astype(jnp.float32) + mlp_sum).astype(jnp.bfloat16)


def swap(value, axis):
    return lax.ppermute(value, axis, [(0, 1), (1, 0)])


def in_order(first, mine, theirs):
    return jnp.stack([jnp.where(first, mine, theirs), jnp.where(first, theirs, mine)])


def scaled_dot(rows, weight):
    return jnp.dot(rows, weight, preferred_element_type=jnp.float32)


def paired_body(
    input_activation_entries,
    premixing_rescale_factor,
    probe_weight_table,
    probe_factor_list,
    lookup_weight_table,
    lookup_factor_list,
    forget_weight_table,
    forget_factor_list,
    forget_shift_term,
    extra_forget_logs,
    content_weight_table,
    content_factor_list,
    filter_weight_table,
    filter_factor_list,
    per_group_rescale_factor,
    emission_weight_table,
    emission_factor_list,
    perceptron_prenorm_factor,
    raising_weight_table,
    raising_factor_list,
    lowering_weight_table,
    lowering_factor_list,
):
    side = lax.axis_index("y")
    mine = 2 * lax.axis_index("rep") + side
    core = lax.axis_index("tp")
    first_core = core == 0
    tokens, width = input_activation_entries.shape
    half = tokens // 2

    def share(tensor, axis, who=mine):
        extent = tensor.shape[axis] // GROUP
        return lax.dynamic_slice_in_dim(tensor, who * extent, extent, axis)

    def across(value, distance):
        return lax.ppermute(value, ("rep", "y"), [(i, i ^ distance) for i in range(GROUP)])

    def shared(rows):
        pieces = jnp.stack([rows] + [across(rows, d) for d in range(1, GROUP)])
        pieces = in_order(first_core, pieces, swap(pieces, "tp"))
        return pieces.transpose(1, 0, 2, 3).reshape(GROUP * tokens, width)

    def half_rows(tensor, who=core):
        return lax.dynamic_slice_in_dim(tensor, who * half, half, tensor.ndim - 2)

    scales = lax.all_gather(
        jnp.stack([emission_factor_list, lowering_factor_list]), ("z", "y"), axis=1, tiled=True
    )
    def gathered(tables, cut, joined, along):
        def piece(who):
            shares = [share(table, cut, who).astype(jnp.bfloat16) for table in tables]
            return jnp.concatenate(shares, axis=joined)

        pair = in_order(side == 0, piece(mine), swap(piece(mine ^ 1), "y"))
        pair = jnp.concatenate([pair[0], pair[1]], axis=along)
        return lax.all_gather(pair, "z", axis=along, tiled=True)

    entry_whole = gathered(
        (
            probe_weight_table,
            lookup_weight_table,
            forget_weight_table,
            content_weight_table,
            filter_weight_table,
        ),
        1,
        1,
        0,
    )
    exits_whole = gathered((emission_weight_table, lowering_weight_table), 0, 0, 1)
    out_rows = emission_weight_table.shape[0] // GROUP
    out_whole, down_whole = exits_whole[:out_rows], exits_whole[out_rows:]
    up_whole = gathered((raising_weight_table,), 1, 1, 0)

    normed = rms_rows(input_activation_entries, premixing_rescale_factor).astype(jnp.bfloat16)
    both = shared(half_rows(normed))
    bursts = jnp.stack(
        [share(extra_forget_logs, 1)]
        + [across(share(extra_forget_logs, 1, mine ^ d), d) for d in range(1, GROUP)]
    )

    factors = [
        share(factor, 0)
        for factor in (
            probe_factor_list,
            lookup_factor_list,
            forget_factor_list,
            content_factor_list,
            filter_factor_list,
        )
    ]
    projected = scaled_dot(both, entry_whole) * jnp.concatenate(factors)
    pieces, start = [], 0
    for factor in factors:
        stop = start + factor.shape[0]
        pieces.append(projected[:, start:stop].reshape(GROUP, tokens, -1))
        start = stop
    shift, gain = share(forget_shift_term, 0), share(per_group_rescale_factor, 0)
    mixing_product = jax.vmap(
        lambda q, k, d, v, g, b: per_group_mixing_values(q, k, d, v, g, shift, b, gain)
    )(*pieces, bursts)

    def summed(product, weight, scale):
        part = (scaled_dot(product, weight) * scale).astype(jnp.bfloat16).reshape(GROUP, tokens, width)
        theirs = swap(half_rows(part, 1 - core), "tp")
        total = half_rows(part).astype(jnp.float32) + theirs.astype(jnp.float32)
        outgoing = total.astype(jnp.bfloat16)
        result = total[0]
        for d in range(1, GROUP):
            result = result + across(outgoing[d], d).astype(jnp.float32)
        return result

    mix_sum = summed(mixing_product.reshape(GROUP * tokens, -1), out_whole, scales[0])
    entries = half_rows(input_activation_entries)
    residual = (entries.astype(jnp.float32) + mix_sum).astype(jnp.bfloat16)
    normed_mlp = rms_rows(residual, perceptron_prenorm_factor).astype(jnp.bfloat16)
    columns = shared(normed_mlp)
    lifted = scaled_dot(columns, up_whole) * share(raising_factor_list, 0)
    hidden = jnp.square(jax.nn.relu(lifted)).astype(jnp.bfloat16)
    mlp_sum = summed(hidden, down_whole, scales[1])
    layer_half = (residual.astype(jnp.float32) + mlp_sum).astype(jnp.bfloat16)
    return in_order(first_core, layer_half, swap(layer_half, "tp")).reshape(tokens, width)


def specs_over(fs):
    in_specs = (
        P(("rep", *fs), None),
        P(),
        P(fs, "tp"),
        P("tp"),
        P(fs, "tp"),
        P("tp"),
        P(fs, "tp"),
        P("tp"),
        P("tp"),
        P(("rep", *fs), "tp"),
        P(fs, "tp"),
        P("tp"),
        P(fs, "tp"),
        P("tp"),
        P("tp"),
        P("tp", fs),
        P(fs),
        P(),
        P(fs, "tp"),
        P("tp"),
        P("tp", fs),
        P(fs),
    )
    return in_specs, P(("rep", *fs), None)


def solution(mesh):
    sizes = mesh.shape
    plain_in, plain_out = specs_over(("fs",))
    plain = jax.shard_map(
        plain_body, mesh=mesh, in_specs=plain_in, out_specs=plain_out, check_vma=False
    )
    if sizes["rep"] != 2 or sizes["tp"] != 2 or sizes["fs"] % 2:
        return plain
    split_mesh = Mesh(mesh.devices.reshape(2, sizes["fs"] // 2, 2, 2), ("rep", "z", "y", "tp"))
    group_in, group_out = specs_over(("z", "y"))
    grouped = jax.shard_map(
        paired_body, mesh=split_mesh, in_specs=group_in, out_specs=group_out, check_vma=False
    )

    def layer(*arrays):
        heads = arrays[9].shape[1] // sizes["tp"]
        tokens = arrays[0].shape[0] // (sizes["rep"] * sizes["fs"])
        return (plain if heads % GROUP or tokens % 32 else grouped)(*arrays)

    return layer
```
